32 devices in a mesh: grp: 2 (over y), sp: 4 (over z), tp: 4 (over x, core).
Axes of the slice: x: 2, y: 2, z: 4, core: 2. Of those that a mesh axis runs over, the one named last changes fastest.
Arguments:
- stream: bfloat16 [12288, 4096], P(('grp', 'sp', 'tp')), parts along dimension 0, may hold values from -6 to 6
- norm_gain: float32 [2, 4096], replicated, may hold values from 0.1 to 1.9
- mix_weight: bfloat16 [2, 4, 1024, 1024], P(None, None, 'sp', 'tp'), may hold values from -0.1875 to 0.1875
- branch_scale: float32 [2, 4096], replicated, may hold values from 0.1 to 1.9
Outputs:
- result: bfloat16 [12288, 4096], P(('grp', 'sp', 'tp')), parts along dimension 0
The draws below stay inside these ranges and needn't reach their ends.
There are 2 independent parts, one for each index of `grp`. The reference program is written for one: setup_inputs(seed, part) draws one part's arguments, and reference() takes and returns one part's arrays. A program takes and returns all parts, laid end to end along the dimension named above; an argument that names none is the same for every part. Nothing has to cross between parts.
All inputs are finite; a program needn't handle non-finite values.
Results may differ from the reference program's by a relative error of at most 0.0056.
Values may be sent and summed in bfloat16 or wider, within the bound.
A program may use at most 128 MiB of HBM per device.

```python
import jax
import jax.numpy as jnp
from jax import lax

GW = 1024
G = 4
D = 4096
LAYERS = 2
TOKENS = 6144


def block_scale(own_key, shape, split, low, top_value):
    factor_of = 1.0
    for axis_at, blocks in split:
        steps = jax.random.uniform(jax.random.fold_in(jax.random.fold_in(own_key, 6), axis_at), (blocks,), jnp.float32, low / len(split), top_value / len(split))
        factor_of = factor_of * jnp.repeat(jnp.exp(steps), shape[axis_at] // blocks).reshape((-1,) + (1,) * (len(shape) - 1 - axis_at))
    return factor_of


def gaussian(key, shape, scale, bound, cuts=(), kind=jnp.bfloat16):
    loudness = block_scale(key, shape, cuts, -0.22, 0.18) if cuts else 1.0
    values = jax.random.normal(key, shape, jnp.float32) * scale * loudness
    return jnp.minimum(jnp.maximum(values, -bound), bound).astype(kind)


def setup_inputs(seed: int = 0, part: int = 0) -> dict:
    streams_of = jax.random.split(jax.random.key(seed), 5)
    part_splits = jax.random.split(jax.random.fold_in(streams_of[4], part), 5)
    stream = gaussian(part_splits[0], (TOKENS, D), 1.0, 6.0, ((0, 16),))
    norm_gain = jnp.clip(1.0 + 0.18 * jax.random.normal(streams_of[1], (LAYERS, D), jnp.float32), 0.1, 1.9)
    mix_weight = gaussian(streams_of[2], (LAYERS, G, GW, GW), GW ** -0.5, 0.1875, ((2, 4), (3, 4)))
    branch_scale = jnp.clip(1.0 + 0.18 * jax.random.normal(streams_of[3], (LAYERS, D), jnp.float32), 0.1, 1.9)
    return dict(stream=stream, norm_gain=norm_gain, mix_weight=mix_weight, branch_scale=branch_scale)


epsilon = 1e-06
window_lengths = (2, 4, 8, 16)

def trailing_sum(group_block, window_len):
    running = group_block
    for back_step in range(1, window_len):
        shifted = jnp.concatenate([jnp.zeros((back_step, group_block.shape[1]), jnp.float32), group_block[:-back_step]], axis=0)
        running = running + shifted
    return running

def reference(stream, norm_gain, mix_weight, branch_scale):
    residual = stream.astype(jnp.float32)
    counts_base = jnp.arange(TOKENS, dtype=jnp.float32) + 1.0
    for layer_idx in range(LAYERS):
        scale_rows = lax.rsqrt(lax.optimization_barrier(jnp.mean(residual * residual, axis=1, keepdims=True)) + epsilon)
        normed = (residual * scale_rows * norm_gain[layer_idx]).astype(jnp.bfloat16)
        outputs = []
        for group_idx in range(G):
            window_len = window_lengths[group_idx]
            group_block = normed[:, group_idx * GW:(group_idx + 1) * GW].astype(jnp.float32)
            window_mean = trailing_sum(group_block, window_len) / jnp.minimum(counts_base, float(window_len))[:, None]
            pooled = (window_mean - group_block).astype(jnp.bfloat16)
            outputs.append(jnp.dot(pooled, mix_weight[layer_idx, group_idx], preferred_element_type=jnp.float32))
        residual = residual + jnp.concatenate(outputs, axis=1) * branch_scale[layer_idx]
    return residual.astype(jnp.bfloat16)
```

```python
import functools

import jax
import jax.numpy as jnp
from jax import lax
from jax.experimental import pallas as pl
from jax.experimental.pallas import tpu as pltpu
from jax.sharding import PartitionSpec as P

MESH = pl.DeviceIdType.MESH
epsilon = 1e-06
window_lengths = (2, 4, 8, 16)
HALO = 16
LANES = 128


def kernel(X, Z, stream, gain, weight, bscale, out, W, S, R, PO, SC, O, recv, send, local, halo_sem):
    LAYERS, G, K, N = weight.shape
    T = 2 * X
    rows, D = stream.shape
    ext = rows + 2 * HALO
    GW = D // G
    y = lax.axis_index("grp")
    z = lax.axis_index("sp")
    t = lax.axis_index("tp")
    x = t // 2
    c = t % 2
    lin = z * T + t
    t_of = lambda xx: xx * 2 + c
    others = [lax.rem(x + k, X) for k in range(1, X)]
    sources = [lax.rem(x + X - k, X) for k in range(1, X)]
    core_dev = {"tp": t + 1 - 2 * c}
    y_dev = {"grp": 1 - y}
    x_devs = [{"tp": t_of(o)} for o in others]
    next_lin = lin + 1
    prev_lin = lin - 1
    next_dev = {"sp": next_lin // T, "tp": lax.rem(next_lin, T)}
    prev_dev = {"sp": (prev_lin + T) // T - 1, "tp": lax.rem(prev_lin + T, T)}
    has_next = lin < Z * T - 1
    has_prev = lin > 0

    own_rows = pltpu.make_async_copy(stream, S.at[pl.ds(2 * HALO, rows)], local.at[0])
    own_rows.start()

    barrier = pltpu.get_barrier_semaphore()

    def greet(dev):
        pl.semaphore_signal(barrier, inc=1, device_id=dev, device_id_type=MESH)

    greet(core_dev)
    greet(y_dev)
    for dev in x_devs:
        greet(dev)
    for dr in (1, -1):
        @pl.when((z + dr >= 0) & (z + dr < Z))
        def _():
            greet({"sp": z + dr})

    @pl.when(has_next)
    def _():
        greet(next_dev)

    @pl.when(has_prev)
    def _():
        greet(prev_dev)

    one = lambda cond: jnp.where(cond, 1, 0)
    pl.semaphore_wait(
        barrier, 2 + (X - 1) + one(z > 0) + one(z < Z - 1) + one(has_next) + one(has_prev)
    )

    def blk(l, g, s, tt):
        return W.at[l, g, tt, pl.ds(pl.multiple_of(s * K, K), K), :]

    def sem_of(l, g, s, tt):
        return recv.at[((l * G + g) * Z + s) * T + tt]

    sites = 2 * (1 + 1 + (X - 1) + 1 + 3 * X + (X - 1) + 1 + X + 2 * (X - 1))

    def copy(l, d, site, g, s, tt, dev, own=False):
        return pltpu.make_async_remote_copy(
            src_ref=weight.at[l, g] if own else blk(l, g, s, tt),
            dst_ref=blk(l, g, s, tt),
            send_sem=send.at[(l * Z + d) * sites + site],
            recv_sem=sem_of(l, g, s, tt),
            device_id=dev,
            device_id_type=MESH,
        )

    def arrived(l, g, s, tt):
        copy(l, 0, 0, g, s, tt, core_dev).wait_recv()

    def do(mode, *args, **kw):
        if mode == "go":
            copy(*args, **kw).start()
        else:
            copy(*args, **kw).wait_send()

    def need(mode, *args):
        if mode == "go":
            arrived(*args)

    def start(mode, l):
        site = 0
        gA, gA2, gB, gB2 = y, 1 - y, 2 + y, 3 - y
        for i, dr in enumerate((1, -1)):
            @pl.when((z + dr >= 0) & (z + dr < Z))
            def _():
                do(mode, l, 0, 2 * i, gB, z, t, {"sp": z + dr}, own=True)
                do(mode, l, 0, 2 * i + 1, gA, z, t, {"sp": z + dr}, own=True)
        site = 4
        for g in (gA, gA2, gB, gB2):
            for dev in x_devs:
                do(mode, l, 0, site, g, z, t, dev, own=True)
                site += 1
        for g in range(G):
            do(mode, l, 0, site, g, z, t, core_dev, own=True)
            site += 1
        return site

    first_sites = 4 + 4 * (X - 1) + 4
    def round0(mode, l, tick):
        site = first_sites
        for s_x in sources:
            st = t_of(s_x)
            need(mode, l, y, z, st)
            for i, dr in enumerate((1, -1)):
                @pl.when((z + dr >= 0) & (z + dr < Z))
                def _():
                    do(mode, l, 0, site + i, y, z, st, {"sp": z + dr})
            do(mode, l, 0, site + 2, y, z, st, core_dev)
            site += 3
        tick()

    def round0_rest(mode, l):
        site = first_sites + 3 * (X - 1)
        for s_x in sources:
            st = t_of(s_x)
            for g in (1 - y, 2 + y, 3 - y):
                need(mode, l, g, z, st)
                do(mode, l, 0, site, g, z, st, core_dev)
                site += 1
        return site

    def z_part(mode, l, d, tick):
        site = 0
        per = 3 + (X - 1)
        for i, dr in enumerate((1, -1)):
            p = z - dr * d
            @pl.when((p >= 0) & (p < Z))
            def _():
                b = i * per
                g = 2 + y
                need(mode, l, g, p, t)
                @pl.when((z + dr >= 0) & (z + dr < Z))
                def _():
                    do(mode, l, d, b, g, p, t, {"sp": z + dr})
                do(mode, l, d, b + 1, g, p, t, y_dev)
                for k, dev in enumerate(x_devs):
                    do(mode, l, d, b + 2 + k, g, p, t, dev)
                do(mode, l, d, b + 2 + X - 1, g, p, t, core_dev)
        site = 2 * per
        tick()
        for j in range(X):
            u = t_of(lax.rem(x + X - j, X))
            for i, dr in enumerate((1, -1)):
                p = z - dr * d
                @pl.when((p >= 0) & (p < Z))
                def _():
                    b = site + i * 3
                    need(mode, l, y, p, u)
                    @pl.when((z + dr >= 0) & (z + dr < Z))
                    def _():
                        do(mode, l, d, b, y, p, u, {"sp": z + dr})
                    do(mode, l, d, b + 1, y, p, u, y_dev)
                    do(mode, l, d, b + 2, y, p, u, core_dev)
            site += 6
            tick()
            if j == 0:
                for i, dr in enumerate((1, -1)):
                    p = z - dr * d
                    @pl.when((p >= 0) & (p < Z))
                    def _():
                        b = site + i * X
                        g = 3 - y
                        need(mode, l, g, p, t)
                        for k, dev in enumerate(x_devs):
                            do(mode, l, d, b + k, g, p, t, dev)
                        do(mode, l, d, b + X - 1, g, p, t, core_dev)
                site += 2 * X
                tick()
        return site

    z_sites = 2 * (3 + (X - 1)) + 6 * X + 2 * X

    def late_part(mode, l, d, tick):
        per = X + 2 * (X - 1)
        for i, dr in enumerate((1, -1)):
            p = z - dr * d
            @pl.when((p >= 0) & (p < Z))
            def _():
                b = z_sites + i * per
                for j in range(X):
                    u = t_of(lax.rem(x + X - j, X))
                    need(mode, l, 1 - y, p, u)
                    do(mode, l, d, b, 1 - y, p, u, core_dev)
                    b += 1
                for g in (2 + y, 3 - y):
                    for s_x in sources:
                        st = t_of(s_x)
                        need(mode, l, g, p, st)
                        do(mode, l, d, b, g, p, st, core_dev)
                        b += 1
            tick()

    nothing = lambda: None

    def scales_first():
        def body(i, _):
            r = pl.ds(pl.multiple_of(i * 16, 16), 16)
            v = S[r, :].astype(jnp.float32)
            m = jnp.sum(v * v, axis=1, keepdims=True) * (1.0 / D)
            SC[r, :] = jnp.broadcast_to(lax.rsqrt(m + epsilon), (16, LANES))
            return 0
        lax.fori_loop(0, ext // 16, body, 0)

    def scales_next():
        m = jnp.sum(SC[HALO:, :], axis=1, keepdims=True) * (1.0 / D)
        SC[HALO:, :] = jnp.broadcast_to(lax.rsqrt(m + epsilon), (ext - HALO, LANES))

    def pool(l, g):
        w = window_lengths[g]
        lo = HALO * l
        n = ext - lo
        position = lin * rows - 2 * HALO + lo + lax.broadcasted_iota(jnp.int32, (n, LANES), 0)
        inv = 1.0 / jnp.clip((position + 1).astype(jnp.float32), 1.0, float(w))

        def body(i, _):
            cols = pl.ds(pl.multiple_of(g * GW + i * LANES, LANES), LANES)
            v = S[lo:, cols].astype(jnp.float32) if l == 0 else R[lo:, cols]
            v = (v * SC[lo:, :] * gain[l : l + 1, cols]).astype(jnp.bfloat16).astype(jnp.float32)
            run = v
            k = 1
            while k < w:
                run = run + pltpu.roll(run, k, 0)
                k *= 2
            PO[lo:, cols] = (run * inv - v).astype(jnp.bfloat16)
            return 0
        lax.fori_loop(0, GW // LANES, body, 0)

    def peer_arrivals(l, g):
        other = 1 - c
        for s in range(Z):
            for xx in range(X):
                arrived(l, g, s, xx * 2 + other)

    def mix(l, g):
        peer_arrivals(l, g)
        lo = HALO * (l + 1)

        def body(i, _):
            cols = pl.ds(pl.multiple_of(g * GW + i * N, N), N)
            acc = jnp.dot(
                PO[lo:, g * GW : (g + 1) * GW], W[l, g, i], preferred_element_type=jnp.float32
            )
            base = S[lo:, cols].astype(jnp.float32) if l == 0 else R[lo:, cols]
            r = base + acc * bscale[l : l + 1, cols]
            if l == LAYERS - 1:
                O[:, cols] = r.astype(jnp.bfloat16)
            else:
                R[lo:, cols] = r
                sq = r * r
                total = SC[lo:, :]
                for q in range(N // LANES):
                    total = total + sq[:, q * LANES : (q + 1) * LANES]
                SC[lo:, :] = total
            return 0
        lax.fori_loop(0, T, body, 0)
        if l == LAYERS - 1:
            put(g).start()

    def put(g):
        part = pl.ds(g * GW, GW)
        return pltpu.make_async_copy(O.at[:, part], out.at[:, part], local.at[2 + g])

    def own_weights():
        return [
            pltpu.make_async_copy(weight.at[l, g], blk(l, g, z, t), sem_of(l, g, z, t))
            for l in range(LAYERS) for g in range(G)
        ]

    def halo():
        return pltpu.make_async_remote_copy(
            src_ref=stream.at[pl.ds(rows - 2 * HALO, 2 * HALO)],
            dst_ref=S.at[pl.ds(0, 2 * HALO)],
            send_sem=halo_sem.at[0],
            recv_sem=halo_sem.at[1],
            device_id=next_dev,
            device_id_type=MESH,
        )

    @pl.when(has_next)
    def _():
        halo().start()

    start("go", 0)
    for o in own_weights():
        o.start()

    @pl.when(jnp.logical_not(has_prev))
    def _():
        S[0 : 2 * HALO, :] = jnp.zeros((2 * HALO, D), S.dtype)

    unrolled = Z <= 4
    own_rows.wait()

    @pl.when(has_prev)
    def _():
        halo().wait_recv()

    pieces = [scales_first] + [functools.partial(pool, 0, g) for g in range(G)]
    tick_on = [True]

    def tick():
        if pieces and tick_on[0]:
            pieces.pop(0)()

    def flush():
        while pieces:
            pieces.pop(0)()

    def clear_sums():
        SC[...] = jnp.zeros_like(SC)

    def rounds(l):
        round0("go", l, tick)
        if unrolled:
            for d in range(1, Z):
                z_part("go", l, d, tick)
                if d == 1:
                    round0_rest("go", l)
                    if l == 0:
                        start("go", 1)
                if d > 1:
                    late_part("go", l, d - 1, tick)
        else:
            round0_rest("go", l)
            if l == 0:
                start("go", 1)
            lax.fori_loop(1, Z, lambda d, _: (z_part("go", l, d, nothing), 0)[1], 0)

    def drain(l):
        if unrolled:
            late_part("go", l, Z - 1, tick)
        else:
            lax.fori_loop(1, Z, lambda d, _: (late_part("go", l, d, nothing), 0)[1], 0)

    tick()
    tick()
    rounds(0)
    flush()
    for o in own_weights():
        o.wait()
    drain(0)
    pieces.append(clear_sums)
    pieces.extend(functools.partial(mix, 0, g) for g in range(G))
    pieces.append(scales_next)
    pieces.extend(functools.partial(pool, 1, g) for g in range(G))
    rounds(1)
    drain(1)
    flush()
    for g in range(G):
        mix(1, g)

    for l in range(LAYERS):
        start("end", l)
        round0("end", l, nothing)
        round0_rest("end", l)

        def ends(d, _):
            z_part("end", l, d, nothing)
            late_part("end", l, d, nothing)
            return 0
        lax.fori_loop(1, Z, ends, 0)

    @pl.when(has_next)
    def _():
        halo().wait_send()

    for g in range(G):
        put(g).wait()


def solution(mesh):
    Z = mesh.shape["sp"]
    X = mesh.shape["tp"] // 2

    def step(stream, norm_gain, mix_weight, branch_scale):
        rows, D = stream.shape
        layers, G, K, N = mix_weight.shape
        T = 2 * X
        ext = rows + 2 * HALO
        any_space = pl.BlockSpec(memory_space=pl.ANY)
        vmem = pl.BlockSpec(memory_space=pltpu.VMEM)
        sites = 2 * (1 + 1 + (X - 1) + 1 + 3 * X + (X - 1) + 1 + X + 2 * (X - 1))
        return pl.pallas_call(
            functools.partial(kernel, X, Z),
            out_shape=jax.ShapeDtypeStruct((rows, D), stream.dtype),
            in_specs=[any_space, vmem, any_space, vmem],
            out_specs=any_space,
            scratch_shapes=[
                pltpu.VMEM((layers, G, T, K * Z, N), mix_weight.dtype),
                pltpu.VMEM((ext, D), stream.dtype),
                pltpu.VMEM((ext, D), jnp.float32),
                pltpu.VMEM((ext, D), jnp.bfloat16),
                pltpu.VMEM((ext, LANES), jnp.float32),
                pltpu.VMEM((rows, D), stream.dtype),
                pltpu.SemaphoreType.DMA((layers * G * Z * T,)),
                pltpu.SemaphoreType.DMA((layers * Z * sites,)),
                pltpu.SemaphoreType.DMA((2 + G,)),
                pltpu.SemaphoreType.DMA((2,)),
            ],
            compiler_params=pltpu.CompilerParams(
                collective_id=0, has_side_effects=True, vmem_limit_bytes=60 * 1024 * 1024
            ),
        )(stream, norm_gain, mix_weight, branch_scale)

    return jax.shard_map(
        step,
        mesh=mesh,
        in_specs=(P(("grp", "sp", "tp"), None), P(), P(None, None, "sp", "tp"), P()),
        out_specs=P(("grp", "sp", "tp"), None),
        check_vma=False,
    )
```

```python
import functools

import jax
import jax.numpy as jnp
from jax import lax
from jax.experimental import pallas as pl
from jax.experimental.pallas import tpu as pltpu
from jax.sharding import PartitionSpec as P

MESH = pl.DeviceIdType.MESH
epsilon = 1e-06
window_lengths = (2, 4, 8, 16)
HALO = 16
LANES = 128


def kernel(X, Z, stream, gain, weight, bscale, O, W, S, R, PO, SC, recv, core_recv, send, local, halo_sem):
    LAYERS, G, K, N = weight.shape
    T = 2 * X
    rows, D = stream.shape
    ext = rows + 2 * HALO
    GW = D // G
    y = lax.axis_index("grp")
    z = lax.axis_index("sp")
    t = lax.axis_index("tp")
    x = t // 2
    c = t % 2
    lin = z * T + t
    t_of = lambda xx: xx * 2 + c
    others = [lax.rem(x + k, X) for k in range(1, X)]
    sources = [lax.rem(x + X - k, X) for k in range(1, X)]
    core_dev = {"tp": t + 1 - 2 * c}
    y_dev = {"grp": 1 - y}
    x_devs = [{"tp": t_of(o)} for o in others]
    next_lin = lin + 1
    prev_lin = lin - 1
    next_dev = {"sp": next_lin // T, "tp": lax.rem(next_lin, T)}
    prev_dev = {"sp": (prev_lin + T) // T - 1, "tp": lax.rem(prev_lin + T, T)}
    has_next = lin < Z * T - 1
    has_prev = lin > 0

    own_rows = pltpu.make_async_copy(stream, S.at[pl.ds(2 * HALO, rows)], local.at[0])
    own_rows.start()

    barrier = pltpu.get_barrier_semaphore()

    def greet(dev):
        pl.semaphore_signal(barrier, inc=1, device_id=dev, device_id_type=MESH)

    greet(core_dev)
    greet(y_dev)
    for dev in x_devs:
        greet(dev)
    for dr in (1, -1):
        @pl.when((z + dr >= 0) & (z + dr < Z))
        def _():
            greet({"sp": z + dr})

    @pl.when(has_next)
    def _():
        greet(next_dev)

    @pl.when(has_prev)
    def _():
        greet(prev_dev)

    one = lambda cond: jnp.where(cond, 1, 0)
    pl.semaphore_wait(
        barrier, 2 + (X - 1) + one(z > 0) + one(z < Z - 1) + one(has_next) + one(has_prev)
    )

    def blk(l, g, s, tt):
        return W.at[l, g, tt, pl.ds(pl.multiple_of(s * K, K), K), :]

    SX, SY, SC0, SZ = 0, 2 * (X - 1), 2 * (X - 1) + 1, 2 * (X - 1) + 2
    per_layer = SZ + 2 * Z

    def sem_of(l, g, s, tt):
        return recv.at[((l * G + g) * Z + s) * X + tt // 2]

    def copy(l, d, link, g, s, tt, dev, own=False):
        return pltpu.make_async_remote_copy(
            src_ref=weight.at[l, g] if own else blk(l, g, s, tt),
            dst_ref=blk(l, g, s, tt),
            send_sem=send.at[l * per_layer + link],
            recv_sem=core_recv.at[l * G + g] if dev is core_dev else sem_of(l, g, s, tt),
            device_id=dev,
            device_id_type=MESH,
        )

    def arrived(l, g, s, tt):
        pltpu.make_async_copy(blk(l, g, s, tt), blk(l, g, s, tt), sem_of(l, g, s, tt)).wait()

    def left(l, link, ref):
        pltpu.make_async_copy(ref, ref, send.at[l * per_layer + link]).wait()

    def go(*args, **kw):
        copy(*args, **kw).start()

    def zlink(i, d):
        return SZ + 2 * d + i

    def start(l):
        for i, dr in enumerate((1, -1)):
            @pl.when((z + dr >= 0) & (z + dr < Z))
            def _():
                go(l, 0, zlink(i, 0), 2 + y, z, t, {"sp": z + dr}, own=True)
                go(l, 0, zlink(i, 0), y, z, t, {"sp": z + dr}, own=True)
        for g in (y, 1 - y, 2 + y, 3 - y):
            for k, dev in enumerate(x_devs):
                go(l, 0, SX + 2 * k, g, z, t, dev, own=True)
        for g in range(G):
            go(l, 0, SC0, g, z, t, core_dev, own=True)

    def round0(l, tick):
        for s_x in sources:
            st = t_of(s_x)
            arrived(l, y, z, st)
            for i, dr in enumerate((1, -1)):
                @pl.when((z + dr >= 0) & (z + dr < Z))
                def _():
                    go(l, 0, zlink(i, 0), y, z, st, {"sp": z + dr})
            go(l, 0, SC0, y, z, st, core_dev)
        tick()

    def round0_rest(l):
        for s_x in sources:
            st = t_of(s_x)
            for g in (1 - y, 2 + y, 3 - y):
                arrived(l, g, z, st)
                go(l, 0, SC0, g, z, st, core_dev)

    def z_part(l, d, tick):
        for i, dr in enumerate((1, -1)):
            p = z - dr * d
            @pl.when((p >= 0) & (p < Z))
            def _():
                g = 2 + y
                arrived(l, g, p, t)
                @pl.when((z + dr >= 0) & (z + dr < Z))
                def _():
                    go(l, d, zlink(i, d), g, p, t, {"sp": z + dr})
                go(l, d, SY, g, p, t, y_dev)
                for k, dev in enumerate(x_devs):
                    go(l, d, SX + 2 * k + 1, g, p, t, dev)
                go(l, d, SC0, g, p, t, core_dev)
        tick()
        for j in range(X):
            u = t_of(lax.rem(x + X - j, X))
            for i, dr in enumerate((1, -1)):
                p = z - dr * d
                @pl.when((p >= 0) & (p < Z))
                def _():
                    arrived(l, y, p, u)
                    @pl.when((z + dr >= 0) & (z + dr < Z))
                    def _():
                        go(l, d, zlink(i, d), y, p, u, {"sp": z + dr})
                    go(l, d, SY, y, p, u, y_dev)
                    go(l, d, SC0, y, p, u, core_dev)
            tick()
            if j == 0:
                for i, dr in enumerate((1, -1)):
                    p = z - dr * d
                    @pl.when((p >= 0) & (p < Z))
                    def _():
                        g = 3 - y
                        arrived(l, g, p, t)
                        for k, dev in enumerate(x_devs):
                            go(l, d, SX + 2 * k + 1, g, p, t, dev)
                        go(l, d, SC0, g, p, t, core_dev)
                tick()

    def late_part(l, d, tick, parts="yx"):
        for i, dr in enumerate((1, -1)):
            p = z - dr * d
            @pl.when((p >= 0) & (p < Z))
            def _():
                for j in range(X) if "y" in parts else ():
                    u = t_of(lax.rem(x + X - j, X))
                    arrived(l, 1 - y, p, u)
                    go(l, d, SC0, 1 - y, p, u, core_dev)
                for g in (2 + y, 3 - y) if "x" in parts else ():
                    for s_x in sources:
                        st = t_of(s_x)
                        arrived(l, g, p, st)
                        go(l, d, SC0, g, p, st, core_dev)
            tick()

    def sent(l):
        for k in range(X - 1):
            left(l, SX + 2 * k, W.at[l, :, 0, pl.ds(0, K)])
            left(l, SX + 2 * k + 1, W.at[l, pl.ds(0, 2), 0, pl.ds(0, (Z - 1) * K)])
        left(l, SY, W.at[l, 0, pl.ds(0, X + 1), pl.ds(0, (Z - 1) * K)])
        left(l, SC0, W.at[l, :, pl.ds(0, X)])
        for d in range(Z):
            for i, dr in enumerate((1, -1)):
                p = z - dr * d
                @pl.when((p >= 0) & (p < Z) & (z + dr >= 0) & (z + dr < Z))
                def _():
                    left(l, zlink(i, d), W.at[l, 0, pl.ds(0, X + 1), pl.ds(0, K)])

    nothing = lambda: None

    def scales_first():
        def body(i, _):
            r = pl.ds(pl.multiple_of(i * 16, 16), 16)
            v = S[r, :].astype(jnp.float32)
            m = jnp.sum(v * v, axis=1, keepdims=True) * (1.0 / D)
            SC[r, :] = jnp.broadcast_to(lax.rsqrt(m + epsilon), (16, LANES))
            return 0
        lax.fori_loop(0, ext // 16, body, 0)

    def scales_next():
        m = jnp.sum(SC[HALO:, :], axis=1, keepdims=True) * (1.0 / D)
        SC[HALO:, :] = jnp.broadcast_to(lax.rsqrt(m + epsilon), (ext - HALO, LANES))

    def pool(l, g):
        w = window_lengths[g]
        lo = HALO * l
        n = ext - lo
        position = lin * rows - 2 * HALO + lo + lax.broadcasted_iota(jnp.int32, (n, LANES), 0)
        inv = 1.0 / jnp.clip((position + 1).astype(jnp.float32), 1.0, float(w))

        def body(i, _):
            cols = pl.ds(pl.multiple_of(g * GW + i * LANES, LANES), LANES)
            v = S[lo:, cols].astype(jnp.float32) if l == 0 else R[lo:, cols]
            v = (v * SC[lo:, :] * gain[l : l + 1, cols]).astype(jnp.bfloat16).astype(jnp.float32)
            run = v
            k = 1
            while k < w:
                run = run + pltpu.roll(run, k, 0)
                k *= 2
            PO[lo:, cols] = (run * inv - v).astype(jnp.bfloat16)
            return 0
        lax.fori_loop(0, GW // LANES, body, 0)

    def peer_arrivals(l, g):
        ref = W.at[l, g, pl.ds(0, X)]
        pltpu.make_async_copy(ref, ref, core_recv.at[l * G + g]).wait()

    def mix(l, g):
        peer_arrivals(l, g)
        lo = HALO * (l + 1)

        def body(i, _):
            cols = pl.ds(pl.multiple_of(g * GW + i * N, N), N)
            acc = jnp.dot(
                PO[lo:, g * GW : (g + 1) * GW], W[l, g, i], preferred_element_type=jnp.float32
            )
            base = S[lo:, cols].astype(jnp.float32) if l == 0 else R[lo:, cols]
            r = base + acc * bscale[l : l + 1, cols]
            if l == LAYERS - 1:
                O[:, cols] = r.astype(jnp.bfloat16)
            else:
                R[lo:, cols] = r
                sq = r * r
                total = SC[lo:, :]
                for q in range(N // LANES):
                    total = total + sq[:, q * LANES : (q + 1) * LANES]
                SC[lo:, :] = total
            return 0
        lax.fori_loop(0, T, body, 0)

    def own_weights():
        return [
            pltpu.make_async_copy(weight.at[l, g], blk(l, g, z, t), sem_of(l, g, z, t))
            for l in range(LAYERS) for g in range(G)
        ]

    def halo():
        return pltpu.make_async_remote_copy(
            src_ref=stream.at[pl.ds(rows - 2 * HALO, 2 * HALO)],
            dst_ref=S.at[pl.ds(0, 2 * HALO)],
            send_sem=halo_sem.at[0],
            recv_sem=halo_sem.at[1],
            device_id=next_dev,
            device_id_type=MESH,
        )

    @pl.when(has_next)
    def _():
        halo().start()

    start(0)
    for o in own_weights():
        o.start()

    @pl.when(jnp.logical_not(has_prev))
    def _():
        S[0 : 2 * HALO, :] = jnp.zeros((2 * HALO, D), S.dtype)

    unrolled = Z <= 4
    own_rows.wait()

    @pl.when(has_prev)
    def _():
        halo().wait_recv()

    pieces = [scales_first] + [functools.partial(pool, 0, g) for g in range(G)]
    tick_on = [True]

    def tick():
        if pieces and tick_on[0]:
            pieces.pop(0)()

    def flush():
        while pieces:
            pieces.pop(0)()

    def clear_sums():
        SC[...] = jnp.zeros_like(SC)

    def rounds(l):
        round0(l, tick)
        if unrolled:
            for d in range(1, Z):
                z_part(l, d, tick)
                if d == 1:
                    round0_rest(l)
                if l == 0 and d == 2:
                    start(1)
                if d > 1:
                    late_part(l, d - 1, tick)
        else:
            round0_rest(l)
            if l == 0:
                start(1)
            lax.fori_loop(1, Z, lambda d, _: (z_part(l, d, nothing), 0)[1], 0)

    def drain(l):
        if unrolled:
            late_part(l, Z - 1, tick)
        else:
            lax.fori_loop(1, Z, lambda d, _: (late_part(l, d, nothing), 0)[1], 0)

    tick()
    tick()
    rounds(0)
    flush()
    for o in own_weights():
        o.wait()
    drain(0)
    pieces.append(clear_sums)
    pieces.extend(functools.partial(mix, 0, g) for g in range(G))
    pieces.append(scales_next)
    pieces.extend(functools.partial(pool, 1, g) for g in range(G))
    rounds(1)
    flush()
    if unrolled:
        late_part(1, Z - 1, nothing, "y")
        mix(1, 0)
        mix(1, 1)
        late_part(1, Z - 1, nothing, "x")
    else:
        drain(1)
        mix(1, 0)
        mix(1, 1)
    mix(1, 2)
    mix(1, 3)

    for l in range(LAYERS):
        sent(l)

    @pl.when(has_next)
    def _():
        halo().wait_send()


def solution(mesh):
    Z = mesh.shape["sp"]
    X = mesh.shape["tp"] // 2

    def step(stream, norm_gain, mix_weight, branch_scale):
        rows, D = stream.shape
        layers, G, K, N = mix_weight.shape
        T = 2 * X
        ext = rows + 2 * HALO
        any_space = pl.BlockSpec(memory_space=pl.ANY)
        hbm = pl.BlockSpec(memory_space=pltpu.HBM)
        vmem = pl.BlockSpec(memory_space=pltpu.VMEM)
        return pl.pallas_call(
            functools.partial(kernel, X, Z),
            out_shape=pltpu.VMEM((rows, D), stream.dtype),
            in_specs=[hbm, vmem, hbm, vmem],
            out_specs=vmem,
            scratch_shapes=[
                pltpu.VMEM((layers, G, T, K * Z, N), mix_weight.dtype),
                pltpu.VMEM((ext, D), stream.dtype),
                pltpu.VMEM((ext, D), jnp.float32),
                pltpu.VMEM((ext, D), jnp.bfloat16),
                pltpu.VMEM((ext, LANES), jnp.float32),
                pltpu.SemaphoreType.DMA((layers * G * Z * X,)),
                pltpu.SemaphoreType.DMA((layers * G,)),
                pltpu.SemaphoreType.DMA((layers * (2 * X + 2 * Z),)),
                pltpu.SemaphoreType.DMA((1,)),
                pltpu.SemaphoreType.DMA((2,)),
            ],
            compiler_params=pltpu.CompilerParams(
                collective_id=0, has_side_effects=True, vmem_limit_bytes=60 * 1024 * 1024
            ),
        )(stream, norm_gain, mix_weight, branch_scale)

    return jax.shard_map(
        step,
        mesh=mesh,
        in_specs=(P(("grp", "sp", "tp"), None), P(), P(None, None, "sp", "tp"), P()),
        out_specs=P(("grp", "sp", "tp"), None),
        check_vma=False,
    )
```
